32 devices in a mesh: sp: 4 (over z), fs: 4 (over y, x), tp: 2 (over core).
Axes of the slice: x: 2, y: 2, z: 4, core: 2. Of those that a mesh axis runs over, the one named last changes fastest.
Arguments:
- activations: bfloat16 [4, 1024, 2048], P('fs', 'sp'), may hold values from -600 to 600
- norm_gain: float32 [2048], replicated, may hold values from 0.1 to 1.9
- w_conv_gate: bfloat16 [2048, 1024], P('sp', ('fs', 'tp')), may hold values from -0.125 to 0.125
- w_conv_mult: bfloat16 [2048, 1024], P('sp', ('fs', 'tp')), may hold values from -0.125 to 0.125
- w_conv_in: bfloat16 [2048, 1024], P('sp', ('fs', 'tp')), may hold values from -0.125 to 0.125
- conv_taps: float32 [3, 1024], replicated, may hold values from -3.5 to 3.5
- w_query: bfloat16 [2048, 1024], P('sp', ('fs', 'tp')), may hold values from -0.125 to 0.125
- w_key: bfloat16 [2048, 1024], P('sp', ('fs', 'tp')), may hold values from -0.125 to 0.125
- w_value: bfloat16 [2048, 1024], P('sp', ('fs', 'tp')), may hold values from -0.125 to 0.125
- w_input_gate: bfloat16 [2048, 8], replicated, may hold values from -0.125 to 0.125
- w_forget_gate: bfloat16 [2048, 8], replicated, may hold values from -0.125 to 0.125
- gate_bias: float32 [2, 8], replicated, may hold values from -1 to 120
- decay_shift: float32 [4, 1024, 8], P(None, 'sp'), may hold values from -2 to 0, as said below
- head_gain: float32 [1024], replicated, may hold values from 0.1 to 1.9
- w_out_conv: bfloat16 [1024, 2048], P(('fs', 'tp'), 'sp'), may hold values from -0.125 to 0.125
- w_out_mem: bfloat16 [1024, 2048], P(('fs', 'tp'), 'sp'), may hold values from -0.125 to 0.125
Outputs:
- output: bfloat16 [4, 1024, 2048], P('fs', ('sp', 'tp'))
The draws below stay inside these ranges and needn't reach their ends.
Inputs may be any that keep to these rules, and one draw needn't show every extreme that they name: `decay_shift`: never positive.
All inputs are finite; a program needn't handle non-finite values.
Results may differ from the reference program's by a relative error of at most 0.015.
Values may be sent and summed in bfloat16 or wider, within the bound.
A program may use at most 64 MiB of HBM per device.

```python
import math
import jax
import jax.numpy as jnp
from jax import lax

D = 2048
CONV_CH = 1024
MEMORY_HEADS = 8
HEAD_DIM = 128
BLOCK = 64
TAPS = 3
TOK_DEV = 256
SEQUENCE_COUNT = 4
SEQUENCE_LENGTH = 1024


def draw_activations(key, part):
    random_subkeys = jax.random.split(key, 3)
    row_scale = jnp.exp(jax.random.uniform(random_subkeys[0], (SEQUENCE_COUNT, SEQUENCE_LENGTH, 1), jnp.float32, 0.0, math.log(10.0)))
    col_scale = jnp.exp(jax.random.uniform(random_subkeys[1], (1, 1, D), jnp.float32, 0.0, math.log(10.0)))
    base_values = jnp.clip(jax.random.normal(random_subkeys[2], (SEQUENCE_COUNT, SEQUENCE_LENGTH, D), jnp.float32), -6.0, 6.0)
    return (base_values * row_scale * col_scale).astype(jnp.bfloat16)


def draw_gate_bias(key, part):
    random_subkeys = jax.random.split(key, 4)
    ranking = jax.random.permutation(random_subkeys[0], MEMORY_HEADS)
    slow_heads = ranking < MEMORY_HEADS // 2
    entry_bias = jax.random.uniform(random_subkeys[1], (MEMORY_HEADS,), jnp.float32, -1.0, 1.0)
    slow_bias = math.log(SEQUENCE_LENGTH) + 2.0 + jax.random.uniform(random_subkeys[2], (MEMORY_HEADS,), jnp.float32, -0.3, 0.3)
    fast_bias = jax.random.uniform(random_subkeys[3], (MEMORY_HEADS,), jnp.float32, 3.0, 4.5)
    forget = jnp.where(slow_heads, slow_bias, fast_bias)
    return jnp.stack([entry_bias, forget], axis=0)


def draw_decay_shift(key, part):
    random_subkeys = jax.random.split(key, 3)
    nblocks = SEQUENCE_LENGTH // TOK_DEV
    low_rate, high_rate = (0.2, 2.0)
    rates = jnp.exp(jax.random.uniform(random_subkeys[0], (SEQUENCE_COUNT, nblocks, 1, MEMORY_HEADS), jnp.float32, math.log(low_rate), math.log(high_rate)))
    stable_part = -jnp.broadcast_to(rates, (SEQUENCE_COUNT, nblocks, TOK_DEV, MEMORY_HEADS)).reshape(SEQUENCE_COUNT, SEQUENCE_LENGTH, MEMORY_HEADS) / SEQUENCE_LENGTH
    spike_positions = jax.random.randint(random_subkeys[1], (SEQUENCE_COUNT, 2, MEMORY_HEADS), 0, SEQUENCE_LENGTH)
    spike_penalty = jax.random.uniform(random_subkeys[2], (SEQUENCE_COUNT, 2, MEMORY_HEADS), jnp.float32, 0.2, 0.5)
    chosen_positions = jnp.arange(SEQUENCE_LENGTH)[None, :, None, None]
    match_count = (chosen_positions == spike_positions[:, None, :, :]).astype(jnp.float32)
    spike_events = jnp.sum(match_count * jnp.log(1.0 - spike_penalty)[:, None, :, :], axis=2)
    return stable_part + spike_events


def steps_of(stream_key, shape, cuts, least, largest):
    gain, own = 1.0, jax.random.fold_in(stream_key, 6)
    for axis_at, parts in cuts:
        steps = jnp.exp(jax.random.uniform(jax.random.fold_in(own, axis_at), (parts,), jnp.float32, least / len(cuts), largest / len(cuts)))
        gain = gain * jnp.repeat(steps, shape[axis_at] // parts).reshape([-1 if axis == axis_at else 1 for axis in range(len(shape))])
    return gain


def gaussian(rng, dims, deviation, bound, cuts=(), held_as=jnp.bfloat16):
    entries = jax.random.normal(rng, dims, jnp.float32) * deviation
    if len(cuts) > 0:
        entries = steps_of(rng, dims, cuts, -0.22, 0.18) * entries
    return jnp.clip(entries, min=-bound, max=bound).astype(held_as)


def setup_inputs(seed: int = 0) -> dict:
    splits = jax.random.split(jax.random.key(seed), 17)
    return {
        "activations": draw_activations(jax.random.fold_in(splits[16], 71), 0),
        "norm_gain": jnp.clip(1.0 + 0.18 * jax.random.normal(splits[1], (D,), jnp.float32), 0.1, 1.9),
        "w_conv_gate": gaussian(splits[2], (D, CONV_CH), D ** -0.5, 0.125, ((0, 4), (1, 8))),
        "w_conv_mult": gaussian(splits[3], (D, CONV_CH), D ** -0.5, 0.125, ((0, 4), (1, 8))),
        "w_conv_in": gaussian(splits[4], (D, CONV_CH), D ** -0.5, 0.125, ((0, 4), (1, 8))),
        "conv_taps": gaussian(splits[5], (TAPS, CONV_CH), TAPS ** -0.5, 3.5, (), jnp.float32),
        "w_query": gaussian(splits[6], (D, MEMORY_HEADS * HEAD_DIM), D ** -0.5, 0.125, ((0, 4), (1, 8))),
        "w_key": gaussian(splits[7], (D, MEMORY_HEADS * HEAD_DIM), D ** -0.5, 0.125, ((0, 4), (1, 8))),
        "w_value": gaussian(splits[8], (D, MEMORY_HEADS * HEAD_DIM), D ** -0.5, 0.125, ((0, 4), (1, 8))),
        "w_input_gate": gaussian(splits[9], (D, MEMORY_HEADS), D ** -0.5, 0.125),
        "w_forget_gate": gaussian(splits[10], (D, MEMORY_HEADS), D ** -0.5, 0.125),
        "gate_bias": draw_gate_bias(jax.random.fold_in(splits[16], 71), 0),
        "decay_shift": draw_decay_shift(jax.random.fold_in(splits[16], 71), 0),
        "head_gain": jnp.clip(1.0 + 0.18 * jax.random.normal(splits[13], (MEMORY_HEADS * HEAD_DIM,), jnp.float32), 0.1, 1.9),
        "w_out_conv": gaussian(splits[14], (CONV_CH, D), (CONV_CH + MEMORY_HEADS * HEAD_DIM) ** -0.5, 0.125, ((0, 8), (1, 4))),
        "w_out_mem": gaussian(splits[15], (MEMORY_HEADS * HEAD_DIM, D), (CONV_CH + MEMORY_HEADS * HEAD_DIM) ** -0.5, 0.125, ((0, 8), (1, 4))),
    }


EPSILON = 1e-06
HIGHEST_PRECISION = lax.Precision.HIGHEST

def combine_states(earlier, later):
    total_one, peak_one, state_one = earlier
    total_two, peak_two, state_two = later
    peak_new = jnp.maximum(total_two + peak_one, peak_two)
    scale_old = jnp.exp(total_two + peak_one - peak_new)
    scale_new = jnp.exp(peak_two - peak_new)
    return (total_one + total_two, peak_new, scale_old[..., None, None] * state_one + scale_new[..., None, None] * state_two)

def head_memory(block_inputs):
    query_rows, key_rows, value_rows, entry_gate, log_forget = block_inputs
    members = query_rows.shape[0]
    tokens = query_rows.shape[1]
    head_width = query_rows.shape[2]
    nblocks = tokens // BLOCK
    block_shape = (members, nblocks, BLOCK, head_width)
    query_blocks = query_rows.astype(jnp.float32).reshape(block_shape)
    key_blocks = key_rows.astype(jnp.float32).reshape(block_shape) * head_width ** (-0.5)
    value_blocks = value_rows.astype(jnp.float32).reshape(block_shape)
    entry_blocks = entry_gate.reshape(members, nblocks, BLOCK)
    forget_sums = jnp.cumsum(log_forget.reshape(members, nblocks, BLOCK), axis=-1)
    block_total = forget_sums[..., -1]
    local_logs = block_total[..., None] - forget_sums + entry_blocks
    local_peak = lax.optimization_barrier(jnp.max(local_logs, axis=-1))
    local_weights = jnp.exp(local_logs - local_peak[..., None])
    local_state = jnp.einsum('bclv,bclk->bcvk', local_weights[..., None] * value_blocks, key_blocks, precision=HIGHEST_PRECISION)

    def advance(running, block_item):
        return (combine_states(running, block_item), running)
    anchor = (jnp.zeros((members,), jnp.float32), jnp.zeros((members,), jnp.float32), jnp.zeros((members, head_width, head_width), jnp.float32))
    block_items = (jnp.moveaxis(block_total, 1, 0), jnp.moveaxis(local_peak, 1, 0), jnp.moveaxis(local_state, 1, 0))
    _, prior_states = lax.scan(advance, anchor, block_items)
    prior_peak = jnp.moveaxis(prior_states[1], 0, 1)
    prior_state = jnp.moveaxis(prior_states[2], 0, 1)
    positions = jnp.arange(BLOCK)
    causal_mask = positions[:, None] >= positions[None, :]
    pair_logs = jnp.where(causal_mask, forget_sums[..., :, None] - forget_sums[..., None, :] + entry_blocks[..., None, :], -jnp.inf)
    carried_logs = forget_sums + prior_peak[..., None]
    row_peak = jnp.maximum(carried_logs, lax.optimization_barrier(jnp.max(pair_logs, axis=-1)))
    inner_weights = jnp.exp(pair_logs - row_peak[..., None])
    carried_weights = jnp.exp(carried_logs - row_peak)
    scores = inner_weights * jnp.einsum('bcld,bcsd->bcls', query_blocks, key_blocks, precision=HIGHEST_PRECISION)
    numerator = carried_weights[..., None] * jnp.einsum('bcvk,bclk->bclv', prior_state, query_blocks, precision=HIGHEST_PRECISION) + jnp.einsum('bcls,bcsv->bclv', scores, value_blocks, precision=HIGHEST_PRECISION)
    return numerator.reshape(members, tokens, head_width)

def reference(activations, norm_gain, w_conv_gate, w_conv_mult, w_conv_in, conv_taps, w_query, w_key, w_value, w_input_gate, w_forget_gate, gate_bias, decay_shift, head_gain, w_out_conv, w_out_mem):
    seq_count = activations.shape[0]
    length = activations.shape[1]
    model_width = activations.shape[2]
    flat_rows = activations.reshape(seq_count * length, model_width).astype(jnp.float32)
    normed = (flat_rows * lax.rsqrt(lax.optimization_barrier(jnp.mean(flat_rows * flat_rows, axis=-1, keepdims=True)) + EPSILON) * norm_gain).astype(jnp.bfloat16)

    def project(weight):
        return jnp.dot(normed, weight, preferred_element_type=jnp.float32).astype(jnp.bfloat16)
    conv_gate = project(w_conv_gate).reshape(seq_count, length, CONV_CH)
    conv_mult = project(w_conv_mult).reshape(seq_count, length, CONV_CH)
    conv_in = project(w_conv_in).reshape(seq_count, length, CONV_CH)
    product = (conv_mult.astype(jnp.float32) * conv_in.astype(jnp.float32)).astype(jnp.bfloat16)
    padded = jnp.pad(product, ((0, 0), (TAPS - 1, 0), (0, 0))).astype(jnp.float32)
    mixed_sum = jnp.zeros((seq_count, length, CONV_CH), jnp.float32)
    for tap_index in range(TAPS):
        mixed_sum = mixed_sum + conv_taps[tap_index] * padded[:, tap_index:tap_index + length, :]
    conv_out = (conv_gate.astype(jnp.float32) * mixed_sum).astype(jnp.bfloat16)

    def heads_first(values, inner):
        return jnp.moveaxis(values.reshape(seq_count, length, MEMORY_HEADS, inner), 2, 0)
    query_heads = heads_first(project(w_query), HEAD_DIM)
    key_heads = heads_first(project(w_key), HEAD_DIM)
    value_heads = heads_first(project(w_value), HEAD_DIM)
    entry = jnp.dot(normed, w_input_gate, preferred_element_type=jnp.float32) + gate_bias[0]
    log_forget = jax.nn.log_sigmoid(jnp.dot(normed, w_forget_gate, preferred_element_type=jnp.float32) + gate_bias[1]) + decay_shift.reshape(seq_count * length, MEMORY_HEADS)
    entry_heads = jnp.moveaxis(entry.reshape(seq_count, length, MEMORY_HEADS), 2, 0)
    forget_heads = jnp.moveaxis(log_forget.reshape(seq_count, length, MEMORY_HEADS), 2, 0)
    memory = lax.map(head_memory, (query_heads, key_heads, value_heads, entry_heads, forget_heads))
    memory = memory * lax.rsqrt(lax.optimization_barrier(jnp.mean(memory * memory, axis=-1, keepdims=True)) + EPSILON) * head_gain.reshape(MEMORY_HEADS, 1, 1, HEAD_DIM)
    mem_out = jnp.moveaxis(memory, 0, 2).reshape(seq_count * length, MEMORY_HEADS * HEAD_DIM).astype(jnp.bfloat16)
    output = jnp.dot(conv_out.reshape(seq_count * length, CONV_CH), w_out_conv, preferred_element_type=jnp.float32) + jnp.dot(mem_out, w_out_mem, preferred_element_type=jnp.float32)
    return output.astype(jnp.bfloat16).reshape(seq_count, length, model_width)
```

```python
import functools

import jax
import jax.numpy as jnp
from jax import lax
from jax.experimental import pallas as pl
from jax.experimental.pallas import tpu as pltpu
from jax.sharding import PartitionSpec as P

MEMORY_HEADS = 8
HEAD_DIM = 128
BLOCK = 64


EPSILON = 1e-06
FAR_BELOW = -1e30
HIGHEST_PRECISION = lax.Precision.HIGHEST


def prefix(value, axis, join, neutral):
    count, mine = (lax.axis_size(axis), lax.axis_index(axis))
    pieces = jax.tree.map(lambda part: lax.all_gather(part, axis), value)
    subtotal = jax.tree.map(
        lambda part, zero: jnp.full_like(part, 0) + jnp.asarray(zero, part.dtype), value, neutral
    )

    def lap(position, subtotal):
        longer = join(subtotal, jax.tree.map(lambda part: part[position], pieces))
        return jax.tree.map(lambda new, old: jnp.where(position < mine, new, old), longer, subtotal)

    return lax.fori_loop(0, count - 1, lap, subtotal)


def from_behind(array, axis, by):
    peers = lax.axis_size(axis)
    pairs = [(i, i + by) for i in range(peers) if 0 <= i + by < peers]
    return lax.ppermute(array, axis, pairs)


def combine_states(earlier, later):
    total_one, peak_one, state_one = earlier
    total_two, peak_two, state_two = later
    peak_new = jnp.maximum(total_two + peak_one, peak_two)
    scale_old = jnp.exp(total_two + peak_one - peak_new)
    scale_new = jnp.exp(peak_two - peak_new)
    return (
        total_one + total_two,
        peak_new,
        scale_old[..., None, None] * state_one + scale_new[..., None, None] * state_two,
    )


def head_rows(values, seq_count, heads_here):
    tokens = values.shape[1]
    split_heads = values.reshape(seq_count, tokens, heads_here, HEAD_DIM).transpose(0, 2, 1, 3)
    return split_heads.reshape(seq_count * heads_here, tokens, HEAD_DIM).astype(jnp.float32)


def gate_rows(values, seq_count, heads_here):
    tokens = values.shape[1]
    return values.transpose(0, 2, 1).reshape(seq_count * heads_here, tokens)


def memory_cell(query_rows, key_rows, value_rows, entry_gate, log_forget):
    members = query_rows.shape[0]
    tokens = query_rows.shape[1]
    head_width = query_rows.shape[2]
    nblocks = tokens // BLOCK
    block_shape = (members, nblocks, BLOCK, head_width)
    query_blocks = query_rows.reshape(block_shape)
    key_blocks = key_rows.reshape(block_shape) * head_width ** (-0.5)
    value_blocks = value_rows.reshape(block_shape)
    entry_blocks = entry_gate.reshape(members, nblocks, BLOCK)
    forget_sums = jnp.cumsum(log_forget.reshape(members, nblocks, BLOCK), axis=-1)
    block_total = forget_sums[..., -1]
    local_logs = block_total[..., None] - forget_sums + entry_blocks
    local_peak = jnp.max(local_logs, axis=-1)
    local_weights = jnp.exp(local_logs - local_peak[..., None])
    local_state = jnp.einsum(
        "bclv,bclk->bcvk",
        local_weights[..., None] * value_blocks,
        key_blocks,
        precision=HIGHEST_PRECISION,
    )

    def advance(running, block_item):
        return (combine_states(running, block_item), running)

    zero_sums = jnp.zeros((members,), jnp.float32)
    low_peaks = jnp.full((members,), FAR_BELOW, jnp.float32)
    zero_states = jnp.zeros((members, head_width, head_width), jnp.float32)
    block_items = (
        jnp.moveaxis(block_total, 1, 0),
        jnp.moveaxis(local_peak, 1, 0),
        jnp.moveaxis(local_state, 1, 0),
    )
    device_total, inner_states = lax.scan(advance, (zero_sums, low_peaks, zero_states), block_items)
    inner_states = tuple((jnp.moveaxis(tensor, 0, 1) for tensor in inner_states))
    total_sum, total_peak, total_state = device_total
    before = prefix(
        (total_sum, total_peak, total_state),
        "sp",
        combine_states,
        (zero_sums, low_peaks, zero_states),
    )
    opening = combine_states((zero_sums, zero_sums, zero_states), before)
    opening = tuple((tensor[:, None] for tensor in opening))
    _, prior_peak, prior_state = combine_states(opening, inner_states)
    positions = jnp.arange(BLOCK)
    causal_mask = positions[:, None] >= positions[None, :]
    pair_logs = jnp.where(
        causal_mask,
        forget_sums[..., :, None] - forget_sums[..., None, :] + entry_blocks[..., None, :],
        -jnp.inf,
    )
    carried_logs = forget_sums + prior_peak[..., None]
    row_peak = jnp.maximum(carried_logs, jnp.max(pair_logs, axis=-1))
    inner_weights = jnp.exp(pair_logs - row_peak[..., None])
    carried_weights = jnp.exp(carried_logs - row_peak)
    scores = inner_weights * jnp.einsum(
        "bcld,bcsd->bcls", query_blocks, key_blocks, precision=HIGHEST_PRECISION
    )
    numerator = carried_weights[..., None] * jnp.einsum(
        "bcvk,bclk->bclv", prior_state, query_blocks, precision=HIGHEST_PRECISION
    ) + jnp.einsum("bcls,bcsv->bclv", scores, value_blocks, precision=HIGHEST_PRECISION)
    return numerator.reshape(members, tokens, head_width)


MESH = pl.DeviceIdType.MESH


def greet(peers):
    barrier = pltpu.get_barrier_semaphore()
    total = 0
    for there, peer in peers:
        if there is None:
            pl.semaphore_signal(barrier, inc=1, device_id=peer, device_id_type=MESH)
            total = total + 1
        else:

            @pl.when(there)
            def _(peer=peer):
                pl.semaphore_signal(barrier, inc=1, device_id=peer, device_id_type=MESH)

            total = total + there.astype(jnp.int32)
    pl.semaphore_wait(barrier, total)


def gather_kernel(
    ns,
    nf,
    cuts,
    act_ref,
    gain_ref,
    w0_ref,
    w1_ref,
    w2_ref,
    w3_ref,
    w4_ref,
    w5_ref,
    wg_ref,
    wc_ref,
    wm_ref,
    proj_ref,
    gate_ref,
    wo_ref,
    acts,
    normed,
    wbuf,
    total,
    local_sem,
    a_send,
    a_recv,
    ad_send,
    ad_recv,
    w_send,
    w_recv,
    o_send,
    o_recv,
    p_send,
    p_recv,
    d_send,
    d_recv,
):
    sp, fs, tp = (lax.axis_index("sp"), lax.axis_index("fs"), lax.axis_index("tp"))
    g = fs * 2 + tp
    depth, cols = w0_ref.shape
    width = 6 * cols
    cut = width // cuts
    tokens, model = act_ref.shape
    half = tokens // 2
    ocols = wc_ref.shape[1]
    partner = (sp, fs, 1 - tp)
    has_up, has_down = (sp + 1 < ns, sp > 0)
    up, down = ((sp + 1, fs, tp), (sp - 1, fs, tp))

    own_rows = pl.ds(pl.multiple_of(sp * depth, depth), depth)
    locals_ = []
    for j, ref in enumerate((w0_ref, w1_ref, w2_ref, w3_ref, w4_ref, w5_ref)):
        locals_.append(
            pltpu.make_async_copy(
                ref, wbuf.at[own_rows, pl.ds(j * cols, cols)], local_sem.at[j]
            )
        )
    own_ocols = pl.ds(pl.multiple_of(sp * ocols, ocols), ocols)
    for m, ref in enumerate((wc_ref, wm_ref)):
        locals_.append(
            pltpu.make_async_copy(ref, wo_ref.at[g, m, :, own_ocols], local_sem.at[6 + m])
        )
    locals_.append(pltpu.make_async_copy(act_ref, acts.at[fs], local_sem.at[8]))
    for copy in locals_:
        copy.start()

    fs_peers = [(None, (sp, lax.rem(fs + off, nf), tp)) for off in range(1, nf)]
    greet(fs_peers + [(None, partner), (has_up, up), (has_down, down)])

    my_half = pl.ds(pl.multiple_of(tp * half, half), half)
    other_half = pl.ds(pl.multiple_of((1 - tp) * half, half), half)

    def act_copy(off, src_f):
        return pltpu.make_async_remote_copy(
            act_ref.at[my_half],
            acts.at[src_f, my_half],
            a_send.at[off - 1],
            a_recv.at[off - 1],
            device_id=(sp, lax.rem(fs + off, nf), tp),
            device_id_type=MESH,
        )

    def act_relay(off, src_f, rows):
        return pltpu.make_async_remote_copy(
            acts.at[src_f, rows],
            acts.at[src_f, rows],
            ad_send.at[off - 1],
            ad_recv.at[off - 1],
            device_id=partner,
            device_id_type=MESH,
        )

    def w_copy(side, d, owner, k):
        rows = pl.ds(pl.multiple_of(owner * depth, depth), depth)
        place = wbuf.at[rows, pl.ds(k * cut, cut)]
        return pltpu.make_async_remote_copy(
            place,
            place,
            w_send.at[side, d, k],
            w_recv.at[side, d, k],
            device_id=(up, down)[side],
            device_id_type=MESH,
        )

    def o_copy(side, d, owner):
        place = wo_ref.at[g, :, :, pl.ds(pl.multiple_of(owner * ocols, ocols), ocols)]
        return pltpu.make_async_remote_copy(
            place,
            place,
            o_send.at[side, d],
            o_recv.at[side, d],
            device_id=(up, down)[side],
            device_id_type=MESH,
        )

    def p_copy(owner, off, src_g):
        place = wo_ref.at[src_g, :, :, pl.ds(pl.multiple_of(owner * ocols, ocols), ocols)]
        return pltpu.make_async_remote_copy(
            place,
            place,
            p_send.at[owner, off - 1],
            p_recv.at[owner, off - 1],
            device_id=(sp, lax.rem(fs + off, nf), tp),
            device_id_type=MESH,
        )

    def d_copy(owner, off, src_g):
        place = wo_ref.at[src_g, :, :, pl.ds(pl.multiple_of(owner * ocols, ocols), ocols)]
        return pltpu.make_async_remote_copy(
            place,
            place,
            d_send.at[owner, off],
            d_recv.at[owner, off],
            device_id=partner,
            device_id_type=MESH,
        )

    def origin(off):
        return lax.rem(fs + nf - off, nf)

    def sends(side, d):
        if side == 0:
            return (sp - d >= 0) & has_up
        return (sp + d < ns) & has_down

    def owner_of(side, d):
        return sp - d if side == 0 else sp + d

    def arrives(side, d):
        return (sp - d >= 0) if side == 0 else (sp + d < ns)

    for off in range(1, nf):
        act_copy(off, fs).start()
    for copy in locals_:
        copy.wait()

    def send_z(side, d):
        @pl.when(sends(side, d))
        def _():
            o_copy(side, d, owner_of(side, d)).start()

    def send_w(side, d, k):
        @pl.when(sends(side, d))
        def _():
            w_copy(side, d, owner_of(side, d), k).start()

    for side in range(2):
        send_z(side, 0)
    for k in range(cuts):
        for side in range(2):
            send_w(side, 0, k)

    def spread(owner):
        for off in range(1, nf):
            p_copy(owner, off, g).start()
        d_copy(owner, 0, g).start()

    spread(sp)
    for off in range(1, nf):
        act_copy(off, origin(off)).wait_recv()
        act_relay(off, origin(off), my_half).start()

    def z_round(d):
        for side in range(2):

            @pl.when(arrives(side, d))
            def _():
                owner = owner_of(side, d)
                o_copy(side, d - 1, owner).wait_recv()
                if d < ns - 1:
                    send_z(side, d)
                spread(owner)

    for off in range(1, nf):
        act_relay(off, origin(off), other_half).wait_recv()

    step = 64

    def norm_rows(i, carry):
        f = i // (tokens // step)
        rows = pl.ds(pl.multiple_of(lax.rem(i, tokens // step) * step, step), step)
        x = acts[f, rows, :].astype(jnp.float32)
        scale = lax.rsqrt(jnp.mean(x * x, axis=-1, keepdims=True) + EPSILON)
        out = (x * scale * gain_ref[...]).astype(jnp.bfloat16)
        normed[pl.ds(pl.multiple_of(i * step, step), step), :] = out
        return carry

    lax.fori_loop(0, nf * tokens // step, norm_rows, 0)
    tile = tokens

    def multiply(owner, first):
        rows = pl.ds(pl.multiple_of(owner * depth, depth), depth)

        def body(i, carry):
            here = pl.ds(pl.multiple_of(i * tile, tile), tile)
            part = jnp.dot(
                normed[here, rows], wbuf[rows, :], preferred_element_type=jnp.float32
            )
            total[here, :] = part if first else total[here, :] + part
            return carry

        lax.fori_loop(0, nf, body, 0)

    z_round(1)
    multiply(sp, True)

    def gates(i, carry):
        here = pl.ds(pl.multiple_of(i * tile, tile), tile)
        gate_ref[here, :] = jnp.dot(
            normed[here, :], wg_ref[...], preferred_element_type=jnp.float32
        )
        return carry

    lax.fori_loop(0, nf, gates, 0)

    for d in range(1, ns):
        for k in range(cuts):
            for side in range(2):

                @pl.when(arrives(side, d))
                def _():
                    w_copy(side, d - 1, owner_of(side, d), k).wait_recv()
                    if d < ns - 1:
                        send_w(side, d, k)

        for side in range(2):

            @pl.when(arrives(side, d))
            def _():
                multiply(owner_of(side, d), False)

        if d + 1 < ns:
            z_round(d + 1)

    def round_rows(i, carry):
        here = pl.ds(pl.multiple_of(i * tile, tile), tile)
        proj_ref[here, :] = total[here, :].astype(jnp.bfloat16)
        return carry

    lax.fori_loop(0, nf, round_rows, 0)

    def collect(s, carry):
        for off in range(1, nf):
            src_g = origin(off) * 2 + tp
            p_copy(s, off, src_g).wait_recv()
            d_copy(s, off, src_g).start()
        return carry

    lax.fori_loop(0, ns, collect, 0)

    def finish(s, carry):
        for off in range(nf):
            d_copy(s, off, origin(off) * 2 + 1 - tp).wait_recv()
            d_copy(s, off, origin(off) * 2 + tp).wait_send()
        for off in range(1, nf):
            p_copy(s, off, g).wait_send()
        return carry

    lax.fori_loop(0, ns, finish, 0)
    for off in range(1, nf):
        act_copy(off, fs).wait_send()
        act_relay(off, origin(off), my_half).wait_send()
    for side in range(2):
        for d in range(ns - 1):

            @pl.when(sends(side, d))
            def _():
                o_copy(side, d, owner_of(side, d)).wait_send()
                for k in range(cuts):
                    w_copy(side, d, owner_of(side, d), k).wait_send()


def gather_and_project(act, gain, weights, gate_weights, w_out_conv, w_out_mem):
    ns, nf = (lax.axis_size("sp"), lax.axis_size("fs"))
    tokens, model = act.shape
    depth, cols = weights[0].shape
    rows, ocols = w_out_conv.shape
    count = nf * tokens
    cuts = 2
    vmem = pl.BlockSpec(memory_space=pltpu.VMEM)
    dma = pltpu.SemaphoreType.DMA
    return pl.pallas_call(
        functools.partial(gather_kernel, ns, nf, cuts),
        out_shape=(
            jax.ShapeDtypeStruct((count, 6 * cols), jnp.bfloat16),
            jax.ShapeDtypeStruct((count, gate_weights.shape[1]), jnp.float32),
            jax.ShapeDtypeStruct((nf * 2, 2, rows, ns * ocols), jnp.bfloat16),
        ),
        in_specs=[vmem] * 11,
        out_specs=(vmem, vmem, pl.BlockSpec(memory_space=pl.ANY)),
        scratch_shapes=[
            pltpu.VMEM((nf, tokens, model), jnp.bfloat16),
            pltpu.VMEM((count, model), jnp.bfloat16),
            pltpu.VMEM((ns * depth, 6 * cols), jnp.bfloat16),
            pltpu.VMEM((count, 6 * cols), jnp.float32),
            dma((9,)),
            dma((nf - 1,)),
            dma((nf - 1,)),
            dma((nf - 1,)),
            dma((nf - 1,)),
            dma((2, ns - 1, cuts)),
            dma((2, ns - 1, cuts)),
            dma((2, ns - 1)),
            dma((2, ns - 1)),
            dma((ns, nf - 1)),
            dma((ns, nf - 1)),
            dma((ns, nf)),
            dma((ns, nf)),
        ],
        compiler_params=pltpu.CompilerParams(
            collective_id=0, has_side_effects=True, vmem_limit_bytes=50 * 1024 * 1024
        ),
    )(act, gain, *weights, gate_weights, w_out_conv, w_out_mem)


def output_kernel(nf, mix_ref, wo_ref, out_ref, got, wbuf, acc, w_sem, send, recv, own_sem):
    sp, fs, tp = (lax.axis_index("sp"), lax.axis_index("fs"), lax.axis_index("tp"))
    group = nf * 2
    g = fs * 2 + tp
    loads = [
        pltpu.make_async_copy(wo_ref.at[pl.ds(i * 2, 2)], wbuf.at[pl.ds(i * 2, 2)], w_sem.at[i])
        for i in range(nf)
    ]
    for load in loads:
        load.start()
    own = pltpu.make_async_copy(mix_ref.at[g], got.at[g], own_sem)
    own.start()

    def peer(off):
        to = lax.rem(g + off, group)
        return (sp, to // 2, lax.rem(to, 2))

    greet([(None, peer(off)) for off in range(1, group)])

    def copy(off, to, source):
        return pltpu.make_async_remote_copy(
            mix_ref.at[to],
            got.at[source],
            send.at[off - 1],
            recv.at[off - 1],
            device_id=peer(off),
            device_id_type=MESH,
        )

    for off in range(1, group):
        copy(off, lax.rem(g + off, group), g).start()
    for load in loads:
        load.wait()
    own.wait()

    def add(source, first):
        part = jnp.dot(
            got[source, 0], wbuf[source, 0], preferred_element_type=jnp.float32
        ) + jnp.dot(got[source, 1], wbuf[source, 1], preferred_element_type=jnp.float32)
        acc[...] = part if first else acc[...] + part

    add(g, True)
    for off in range(1, group):
        source = lax.rem(g + group - off, group)
        copy(off, lax.rem(g + off, group), source).wait_recv()
        add(source, False)
    out_ref[...] = acc[...].astype(jnp.bfloat16)
    for off in range(1, group):
        copy(off, lax.rem(g + off, group), g).wait_send()


def exchange_and_merge(mix, wo):
    nf = lax.axis_size("fs")
    group, _, tokens, channels = mix.shape
    width = wo.shape[3]
    vmem = pl.BlockSpec(memory_space=pltpu.VMEM)
    dma = pltpu.SemaphoreType.DMA
    return pl.pallas_call(
        functools.partial(output_kernel, nf),
        out_shape=jax.ShapeDtypeStruct((tokens, width), jnp.bfloat16),
        in_specs=[vmem, pl.BlockSpec(memory_space=pl.ANY)],
        out_specs=vmem,
        scratch_shapes=[
            pltpu.VMEM(mix.shape, jnp.bfloat16),
            pltpu.VMEM(wo.shape, jnp.bfloat16),
            pltpu.VMEM((tokens, width), jnp.float32),
            dma((nf,)),
            dma((group - 1,)),
            dma((group - 1,)),
            dma,
        ],
        compiler_params=pltpu.CompilerParams(
            collective_id=1, has_side_effects=True, vmem_limit_bytes=40 * 1024 * 1024
        ),
    )(mix, wo)


def shards(
    activations,
    norm_gain,
    w_conv_gate,
    w_conv_mult,
    w_conv_in,
    conv_taps,
    w_query,
    w_key,
    w_value,
    w_input_gate,
    w_forget_gate,
    gate_bias,
    decay_shift,
    head_gain,
    w_out_conv,
    w_out_mem,
):
    group_index = lax.axis_index(("fs", "tp"))
    heads_here = MEMORY_HEADS // (lax.axis_size("fs") * lax.axis_size("tp"))
    channels = w_conv_gate.shape[1]
    if lax.axis_size("sp") <= 8 and lax.axis_size("tp") == 2:
        seq_count, tokens = lax.axis_size("fs"), activations.shape[1]
        all_gates = jnp.concatenate([w_input_gate, w_forget_gate], axis=1)
        flat, gate_flat, full_out = gather_and_project(
            activations[0],
            norm_gain[None, :],
            (w_conv_gate, w_conv_mult, w_conv_in, w_query, w_key, w_value),
            all_gates,
            w_out_conv,
            w_out_mem,
        )
        conv_gate, conv_mult, conv_in, query, keys_proj, value = [
            flat[:, at * channels : (at + 1) * channels].reshape(seq_count, tokens, channels)
            for at in range(6)
        ]
        gate_values = jnp.concatenate(
            [
                lax.dynamic_slice_in_dim(
                    gate_flat, at + group_index * heads_here, heads_here, 1
                )
                for at in (0, MEMORY_HEADS)
            ],
            axis=1,
        ).reshape(seq_count, tokens, 2 * heads_here)
    else:
        full_out = None
        sequences = lax.all_gather(activations, "fs", axis=0, tiled=True)
        seq_count = sequences.shape[0]
        tokens = sequences.shape[1]
        model_width = sequences.shape[2]
        row_count = seq_count * tokens
        flat_rows = sequences.reshape(row_count, model_width).astype(jnp.float32)
        normed = (
            flat_rows
            * lax.rsqrt(jnp.mean(flat_rows * flat_rows, axis=-1, keepdims=True) + EPSILON)
            * norm_gain
        ).astype(jnp.bfloat16)
        pieces = (
            lax.all_gather(w_conv_gate, "sp", axis=0, tiled=True),
            lax.all_gather(w_conv_mult, "sp", axis=0, tiled=True),
            lax.all_gather(w_conv_in, "sp", axis=0, tiled=True),
            lax.all_gather(w_query, "sp", axis=0, tiled=True),
            lax.all_gather(w_key, "sp", axis=0, tiled=True),
            lax.all_gather(w_value, "sp", axis=0, tiled=True),
        )
        projected = tuple(
            (jnp.dot(normed, shard_piece, preferred_element_type=jnp.float32) for shard_piece in pieces)
        )
        conv_gate, conv_mult, conv_in, query, keys_proj, value = [
            tensor.astype(jnp.bfloat16).reshape(seq_count, tokens, -1) for tensor in projected
        ]
        entry_cols = lax.dynamic_slice_in_dim(w_input_gate, group_index * heads_here, heads_here, 1)
        forget_cols = lax.dynamic_slice_in_dim(w_forget_gate, group_index * heads_here, heads_here, 1)
        gate_values = jnp.dot(
            normed,
            jnp.concatenate([entry_cols, forget_cols], axis=1),
            preferred_element_type=jnp.float32,
        ).reshape(seq_count, tokens, 2 * heads_here)
    product = (conv_mult.astype(jnp.float32) * conv_in.astype(jnp.float32)).astype(jnp.bfloat16)
    ntaps = conv_taps.shape[0]
    rim_rows = from_behind(product[:, tokens - (ntaps - 1) :, :], "sp", 1)
    padded = jnp.concatenate([rim_rows, product], axis=1).astype(jnp.float32)
    tap_weights = lax.dynamic_slice_in_dim(conv_taps, group_index * channels, channels, 1)
    mixed_sum = jnp.zeros((seq_count, tokens, channels), jnp.float32)
    for tap_index in range(ntaps):
        mixed_sum = (
            mixed_sum + tap_weights[tap_index] * padded[:, tap_index : tap_index + tokens, :]
        )
    conv_out = (conv_gate.astype(jnp.float32) * mixed_sum).astype(jnp.bfloat16)
    bias_rows = lax.dynamic_slice_in_dim(gate_bias, group_index * heads_here, heads_here, 1)
    decay_rows = lax.dynamic_slice_in_dim(decay_shift, group_index * heads_here, heads_here, 2)
    entry = gate_values[..., :heads_here] + bias_rows[0]
    log_forget = jax.nn.log_sigmoid(gate_values[..., heads_here:] + bias_rows[1]) + decay_rows
    cell = memory_cell(
        head_rows(query, seq_count, heads_here),
        head_rows(keys_proj, seq_count, heads_here),
        head_rows(value, seq_count, heads_here),
        gate_rows(entry, seq_count, heads_here),
        gate_rows(log_forget, seq_count, heads_here),
    )
    cell = cell * lax.rsqrt(jnp.mean(cell * cell, axis=-1, keepdims=True) + EPSILON)
    gain_rows = lax.dynamic_slice_in_dim(
        head_gain, group_index * heads_here * HEAD_DIM, heads_here * HEAD_DIM, 0
    ).reshape(1, heads_here, 1, HEAD_DIM)
    scaled = cell.reshape(seq_count, heads_here, tokens, HEAD_DIM) * gain_rows
    mem_out = (
        scaled.transpose(0, 2, 1, 3)
        .reshape(seq_count, tokens, heads_here * HEAD_DIM)
        .astype(jnp.bfloat16)
    )
    if full_out is not None:
        mix = jnp.stack([conv_out, mem_out]).reshape(2, seq_count * 2, tokens // 2, channels)
        merged = exchange_and_merge(mix.transpose(1, 0, 2, 3), full_out)
        return merged[None]
    conv_seq, mem_seq = (
        lax.all_to_all(conv_out, "fs", split_axis=0, concat_axis=2, tiled=True),
        lax.all_to_all(mem_out, "fs", split_axis=0, concat_axis=2, tiled=True),
    )
    rows_conv, rows_mem = (
        lax.all_gather(w_out_conv, "fs", axis=0, tiled=True),
        lax.all_gather(w_out_mem, "fs", axis=0, tiled=True),
    )
    full_conv, full_mem = (
        lax.all_gather(rows_conv, "sp", axis=1, tiled=True),
        lax.all_gather(rows_mem, "sp", axis=1, tiled=True),
    )
    conv_flat = conv_seq[0]
    mem_flat = mem_seq[0]
    output = lax.psum_scatter(
        (
            jnp.dot(conv_flat, full_conv, preferred_element_type=jnp.float32)
            + jnp.dot(mem_flat, full_mem, preferred_element_type=jnp.float32)
        ).astype(jnp.bfloat16),
        "tp",
        scatter_dimension=0,
        tiled=True,
    ).astype(jnp.float32)
    return output.astype(jnp.bfloat16).reshape(1, output.shape[0], -1)


def solution(mesh):
    return jax.shard_map(
        shards,
        mesh=mesh,
        in_specs=(
            P("fs", "sp", None),
            P(),
            P("sp", ("fs", "tp")),
            P("sp", ("fs", "tp")),
            P("sp", ("fs", "tp")),
            P(),
            P("sp", ("fs", "tp")),
            P("sp", ("fs", "tp")),
            P("sp", ("fs", "tp")),
            P(),
            P(),
            P(),
            P(None, "sp", None),
            P(),
            P(("fs", "tp"), "sp"),
            P(("fs", "tp"), "sp"),
        ),
        out_specs=P("fs", ("sp", "tp"), None),
        check_vma=False,
    )
```

```python
import functools

import jax
import jax.numpy as jnp
from jax import lax
from jax.experimental import pallas as pl
from jax.experimental.pallas import tpu as pltpu
from jax.sharding import PartitionSpec as P

MEMORY_HEADS = 8
HEAD_DIM = 128
BLOCK = 64


EPSILON = 1e-06
FAR_BELOW = -1e30
HIGHEST_PRECISION = lax.Precision.HIGHEST


def prefix(value, axis, join, neutral):
    count, mine = (lax.axis_size(axis), lax.axis_index(axis))
    total, peak, state = value
    stats = jnp.stack([total, peak], axis=1)[..., None]
    stats = jnp.broadcast_to(stats, stats.shape[:2] + state.shape[-1:])
    stats = jnp.pad(stats, ((0, 0), (0, 6), (0, 0)))
    packed = lax.all_gather(jnp.concatenate([state, stats], axis=1), axis)
    height = state.shape[1]
    pieces = (packed[:, :, height, 0], packed[:, :, height + 1, 0], packed[:, :, :height])
    subtotal = jax.tree.map(
        lambda part, zero: jnp.full_like(part, 0) + jnp.asarray(zero, part.dtype), value, neutral
    )

    def lap(position, subtotal):
        longer = join(subtotal, jax.tree.map(lambda part: part[position], pieces))
        return jax.tree.map(lambda new, old: jnp.where(position < mine, new, old), longer, subtotal)

    if count <= 8:
        for position in range(count - 1):
            subtotal = lap(position, subtotal)
        return subtotal
    return lax.fori_loop(0, count - 1, lap, subtotal)


def from_behind(array, axis, by):
    peers = lax.axis_size(axis)
    pairs = [(i, i + by) for i in range(peers) if 0 <= i + by < peers]
    return lax.ppermute(array, axis, pairs)


def combine_states(earlier, later):
    total_one, peak_one, state_one = earlier
    total_two, peak_two, state_two = later
    peak_new = jnp.maximum(total_two + peak_one, peak_two)
    scale_old = jnp.exp(total_two + peak_one - peak_new)
    scale_new = jnp.exp(peak_two - peak_new)
    return (
        total_one + total_two,
        peak_new,
        scale_old[..., None, None] * state_one + scale_new[..., None, None] * state_two,
    )


def head_rows(values, seq_count, heads_here):
    tokens = values.shape[1]
    split_heads = values.reshape(seq_count, tokens, heads_here, HEAD_DIM).transpose(0, 2, 1, 3)
    return split_heads.reshape(seq_count * heads_here, tokens, HEAD_DIM).astype(jnp.float32)


def gate_rows(values, seq_count, heads_here):
    tokens = values.shape[1]
    return values.transpose(0, 2, 1).reshape(seq_count * heads_here, tokens)


def memory_cell(query_rows, key_rows, value_rows, entry_gate, log_forget):
    members = query_rows.shape[0]
    tokens = query_rows.shape[1]
    head_width = query_rows.shape[2]
    nblocks = tokens // BLOCK
    block_shape = (members, nblocks, BLOCK, head_width)
    query_blocks = query_rows.reshape(block_shape)
    key_blocks = key_rows.reshape(block_shape) * head_width ** (-0.5)
    value_blocks = value_rows.reshape(block_shape)
    entry_blocks = entry_gate.reshape(members, nblocks, BLOCK)
    forget_sums = jnp.cumsum(log_forget.reshape(members, nblocks, BLOCK), axis=-1)
    block_total = forget_sums[..., -1]
    local_logs = block_total[..., None] - forget_sums + entry_blocks
    local_peak = jnp.max(local_logs, axis=-1)
    local_weights = jnp.exp(local_logs - local_peak[..., None])
    local_state = jnp.einsum(
        "bclv,bclk->bcvk",
        local_weights[..., None] * value_blocks,
        key_blocks,
        precision=HIGHEST_PRECISION,
    )

    def advance(running, block_item):
        return (combine_states(running, block_item), running)

    zero_sums = jnp.zeros((members,), jnp.float32)
    low_peaks = jnp.full((members,), FAR_BELOW, jnp.float32)
    zero_states = jnp.zeros((members, head_width, head_width), jnp.float32)
    block_items = (
        jnp.moveaxis(block_total, 1, 0),
        jnp.moveaxis(local_peak, 1, 0),
        jnp.moveaxis(local_state, 1, 0),
    )
    device_total, inner_states = lax.scan(advance, (zero_sums, low_peaks, zero_states), block_items)
    inner_states = tuple((jnp.moveaxis(tensor, 0, 1) for tensor in inner_states))
    total_sum, total_peak, total_state = device_total
    before = prefix(
        (total_sum, total_peak, total_state),
        "sp",
        combine_states,
        (zero_sums, low_peaks, zero_states),
    )
    opening = combine_states((zero_sums, zero_sums, zero_states), before)
    opening = tuple((tensor[:, None] for tensor in opening))
    _, prior_peak, prior_state = combine_states(opening, inner_states)
    positions = jnp.arange(BLOCK)
    causal_mask = positions[:, None] >= positions[None, :]
    pair_logs = jnp.where(
        causal_mask,
        forget_sums[..., :, None] - forget_sums[..., None, :] + entry_blocks[..., None, :],
        -jnp.inf,
    )
    carried_logs = forget_sums + prior_peak[..., None]
    row_peak = jnp.maximum(carried_logs, jnp.max(pair_logs, axis=-1))
    inner_weights = jnp.exp(pair_logs - row_peak[..., None])
    carried_weights = jnp.exp(carried_logs - row_peak)
    scores = inner_weights * jnp.einsum(
        "bcld,bcsd->bcls", query_blocks, key_blocks, precision=HIGHEST_PRECISION
    )
    numerator = carried_weights[..., None] * jnp.einsum(
        "bcvk,bclk->bclv", prior_state, query_blocks, precision=HIGHEST_PRECISION
    ) + jnp.einsum("bcls,bcsv->bclv", scores, value_blocks, precision=HIGHEST_PRECISION)
    return numerator.reshape(members, tokens, head_width)


MESH = pl.DeviceIdType.MESH


def greet(peers):
    barrier = pltpu.get_barrier_semaphore()
    total = 0
    for there, peer in peers:
        if there is None:
            pl.semaphore_signal(barrier, inc=1, device_id=peer, device_id_type=MESH)
            total = total + 1
        else:

            @pl.when(there)
            def _(peer=peer):
                pl.semaphore_signal(barrier, inc=1, device_id=peer, device_id_type=MESH)

            total = total + there.astype(jnp.int32)
    pl.semaphore_wait(barrier, total)


def gather_kernel(
    ns,
    nf,
    cuts,
    act_ref,
    gain_ref,
    w0_ref,
    w1_ref,
    w2_ref,
    w3_ref,
    w4_ref,
    w5_ref,
    wg_ref,
    wc_ref,
    wm_ref,
    proj_ref,
    gate_ref,
    wo_ref,
    acts,
    normed,
    wbuf,
    total,
    local_sem,
    a_send,
    a_recv,
    ad_send,
    ad_recv,
    w_send,
    w_recv,
    o_send,
    o_recv,
    p_send,
    p_recv,
    d_send,
    d_recv,
):
    sp, fs, tp = (lax.axis_index("sp"), lax.axis_index("fs"), lax.axis_index("tp"))
    g = fs * 2 + tp
    depth, cols = w0_ref.shape
    width = 6 * cols
    cut = width // cuts
    tokens, model = act_ref.shape
    half = tokens // 2
    ocols = wc_ref.shape[1]
    partner = (sp, fs, 1 - tp)
    has_up, has_down = (sp + 1 < ns, sp > 0)
    up, down = ((sp + 1, fs, tp), (sp - 1, fs, tp))

    own_rows = pl.ds(pl.multiple_of(sp * depth, depth), depth)
    locals_ = []
    for j, ref in enumerate((w0_ref, w1_ref, w2_ref, w3_ref, w4_ref, w5_ref)):
        locals_.append(
            pltpu.make_async_copy(
                ref, wbuf.at[own_rows, pl.ds(j * cols, cols)], local_sem.at[j]
            )
        )
    own_ocols = pl.ds(pl.multiple_of(sp * ocols, ocols), ocols)
    for m, ref in enumerate((wc_ref, wm_ref)):
        locals_.append(
            pltpu.make_async_copy(ref, wo_ref.at[g, m, :, own_ocols], local_sem.at[6 + m])
        )
    locals_.append(pltpu.make_async_copy(act_ref, acts.at[fs], local_sem.at[8]))
    for copy in locals_:
        copy.start()

    fs_peers = [(None, (sp, lax.rem(fs + off, nf), tp)) for off in range(1, nf)]
    greet(fs_peers + [(None, partner), (has_up, up), (has_down, down)])

    my_half = pl.ds(pl.multiple_of(tp * half, half), half)
    other_half = pl.ds(pl.multiple_of((1 - tp) * half, half), half)

    def act_copy(off, src_f):
        return pltpu.make_async_remote_copy(
            act_ref.at[my_half],
            acts.at[src_f, my_half],
            a_send.at[off - 1],
            a_recv.at[off - 1],
            device_id=(sp, lax.rem(fs + off, nf), tp),
            device_id_type=MESH,
        )

    def act_relay(off, src_f, rows):
        return pltpu.make_async_remote_copy(
            acts.at[src_f, rows],
            acts.at[src_f, rows],
            ad_send.at[off - 1],
            ad_recv.at[off - 1],
            device_id=partner,
            device_id_type=MESH,
        )

    def w_copy(side, d, owner, k):
        rows = pl.ds(pl.multiple_of(owner * depth, depth), depth)
        place = wbuf.at[rows, pl.ds(k * cut, cut)]
        return pltpu.make_async_remote_copy(
            place,
            place,
            w_send.at[side, d, k],
            w_recv.at[side, d, k],
            device_id=(up, down)[side],
            device_id_type=MESH,
        )

    def o_copy(side, d, owner):
        place = wo_ref.at[g, :, :, pl.ds(pl.multiple_of(owner * ocols, ocols), ocols)]
        return pltpu.make_async_remote_copy(
            place,
            place,
            o_send.at[side, d],
            o_recv.at[side, d],
            device_id=(up, down)[side],
            device_id_type=MESH,
        )

    def p_copy(owner, off, src_g):
        place = wo_ref.at[src_g, :, :, pl.ds(pl.multiple_of(owner * ocols, ocols), ocols)]
        return pltpu.make_async_remote_copy(
            place,
            place,
            p_send.at[owner, off - 1],
            p_recv.at[owner, off - 1],
            device_id=(sp, lax.rem(fs + off, nf), tp),
            device_id_type=MESH,
        )

    def d_copy(owner, off, src_g):
        place = wo_ref.at[src_g, :, :, pl.ds(pl.multiple_of(owner * ocols, ocols), ocols)]
        return pltpu.make_async_remote_copy(
            place,
            place,
            d_send.at[owner, off],
            d_recv.at[owner, off],
            device_id=partner,
            device_id_type=MESH,
        )

    def origin(off):
        return lax.rem(fs + nf - off, nf)

    def sends(side, d):
        if side == 0:
            return (sp - d >= 0) & has_up
        return (sp + d < ns) & has_down

    def owner_of(side, d):
        return sp - d if side == 0 else sp + d

    def arrives(side, d):
        return (sp - d >= 0) if side == 0 else (sp + d < ns)

    for off in range(1, nf):
        act_copy(off, fs).start()
    for copy in locals_:
        copy.wait()

    def send_z(side, d):
        @pl.when(sends(side, d))
        def _():
            o_copy(side, d, owner_of(side, d)).start()

    def send_w(side, d, k):
        @pl.when(sends(side, d))
        def _():
            w_copy(side, d, owner_of(side, d), k).start()

    for side in range(2):
        send_z(side, 0)
    for k in range(cuts):
        for side in range(2):
            send_w(side, 0, k)

    def spread(owner):
        for off in range(1, nf):
            p_copy(owner, off, g).start()
        d_copy(owner, 0, g).start()

    spread(sp)
    for off in range(1, nf):
        act_copy(off, origin(off)).wait_recv()
        act_relay(off, origin(off), my_half).start()

    def z_round(d):
        for side in range(2):

            @pl.when(arrives(side, d))
            def _():
                owner = owner_of(side, d)
                o_copy(side, d - 1, owner).wait_recv()
                if d < ns - 1:
                    send_z(side, d)
                spread(owner)

    for off in range(1, nf):
        act_relay(off, origin(off), other_half).wait_recv()

    step = 64

    def norm_rows(i, carry):
        f = i // (tokens // step)
        rows = pl.ds(pl.multiple_of(lax.rem(i, tokens // step) * step, step), step)
        x = acts[f, rows, :].astype(jnp.float32)
        scale = lax.rsqrt(jnp.mean(x * x, axis=-1, keepdims=True) + EPSILON)
        out = (x * scale * gain_ref[...]).astype(jnp.bfloat16)
        normed[pl.ds(pl.multiple_of(i * step, step), step), :] = out
        return carry

    lax.fori_loop(0, nf * tokens // step, norm_rows, 0)
    tile = tokens

    def multiply(owner, first):
        rows = pl.ds(pl.multiple_of(owner * depth, depth), depth)

        def body(i, carry):
            here = pl.ds(pl.multiple_of(i * tile, tile), tile)
            part = jnp.dot(
                normed[here, rows], wbuf[rows, :], preferred_element_type=jnp.float32
            )
            total[here, :] = part if first else total[here, :] + part
            return carry

        lax.fori_loop(0, nf, body, 0)

    z_round(1)
    multiply(sp, True)

    def gates(i, carry):
        here = pl.ds(pl.multiple_of(i * tile, tile), tile)
        gate_ref[here, :] = jnp.dot(
            normed[here, :], wg_ref[...], preferred_element_type=jnp.float32
        )
        return carry

    lax.fori_loop(0, nf, gates, 0)

    def collect(s, carry):
        for off in range(1, nf):
            src_g = origin(off) * 2 + tp
            p_copy(s, off, src_g).wait_recv()
            d_copy(s, off, src_g).start()
        return carry

    for d in range(1, ns):
        if d == ns - 1:
            lax.fori_loop(0, ns, collect, 0)
        for k in range(cuts):
            for side in range(2):

                @pl.when(arrives(side, d))
                def _():
                    w_copy(side, d - 1, owner_of(side, d), k).wait_recv()
                    if d < ns - 1:
                        send_w(side, d, k)

        for side in range(2):

            @pl.when(arrives(side, d))
            def _():
                multiply(owner_of(side, d), False)

        if d + 1 < ns:
            z_round(d + 1)

    def round_rows(i, carry):
        here = pl.ds(pl.multiple_of(i * tile, tile), tile)
        proj_ref[here, :] = total[here, :].astype(jnp.bfloat16)
        return carry

    lax.fori_loop(0, nf, round_rows, 0)

    def finish(s, carry):
        for off in range(nf):
            d_copy(s, off, origin(off) * 2 + 1 - tp).wait_recv()
            d_copy(s, off, origin(off) * 2 + tp).wait_send()
        for off in range(1, nf):
            p_copy(s, off, g).wait_send()
        return carry

    lax.fori_loop(0, ns, finish, 0)
    for off in range(1, nf):
        act_copy(off, fs).wait_send()
        act_relay(off, origin(off), my_half).wait_send()
    for side in range(2):
        for d in range(ns - 1):

            @pl.when(sends(side, d))
            def _():
                o_copy(side, d, owner_of(side, d)).wait_send()
                for k in range(cuts):
                    w_copy(side, d, owner_of(side, d), k).wait_send()


def gather_and_project(act, gain, weights, gate_weights, w_out_conv, w_out_mem):
    ns, nf = (lax.axis_size("sp"), lax.axis_size("fs"))
    tokens, model = act.shape
    depth, cols = weights[0].shape
    rows, ocols = w_out_conv.shape
    count = nf * tokens
    cuts = 2
    vmem = pl.BlockSpec(memory_space=pltpu.VMEM)
    hbm = pl.BlockSpec(memory_space=pltpu.MemorySpace.HBM)
    dma = pltpu.SemaphoreType.DMA
    return pl.pallas_call(
        functools.partial(gather_kernel, ns, nf, cuts),
        out_shape=(
            jax.ShapeDtypeStruct((count, 6 * cols), jnp.bfloat16),
            jax.ShapeDtypeStruct((count, gate_weights.shape[1]), jnp.float32),
            jax.ShapeDtypeStruct((nf * 2, 2, rows, ns * ocols), jnp.bfloat16),
        ),
        in_specs=[hbm, vmem] + [hbm] * 6 + [vmem, hbm, hbm],
        out_specs=(vmem, vmem, pl.BlockSpec(memory_space=pl.ANY)),
        scratch_shapes=[
            pltpu.VMEM((nf, tokens, model), jnp.bfloat16),
            pltpu.VMEM((count, model), jnp.bfloat16),
            pltpu.VMEM((ns * depth, 6 * cols), jnp.bfloat16),
            pltpu.VMEM((count, 6 * cols), jnp.float32),
            dma((9,)),
            dma((nf - 1,)),
            dma((nf - 1,)),
            dma((nf - 1,)),
            dma((nf - 1,)),
            dma((2, ns - 1, cuts)),
            dma((2, ns - 1, cuts)),
            dma((2, ns - 1)),
            dma((2, ns - 1)),
            dma((ns, nf - 1)),
            dma((ns, nf - 1)),
            dma((ns, nf)),
            dma((ns, nf)),
        ],
        compiler_params=pltpu.CompilerParams(
            collective_id=0, has_side_effects=True, vmem_limit_bytes=50 * 1024 * 1024
        ),
    )(act, gain, *weights, gate_weights, w_out_conv, w_out_mem)


def output_kernel(nf, mix_ref, wo_ref, out_ref, got, wbuf, acc, w_sem, send, recv, own_sem):
    sp, fs, tp = (lax.axis_index("sp"), lax.axis_index("fs"), lax.axis_index("tp"))
    group = nf * 2
    g = fs * 2 + tp
    loads = [
        pltpu.make_async_copy(wo_ref.at[pl.ds(i * 2, 2)], wbuf.at[pl.ds(i * 2, 2)], w_sem.at[i])
        for i in range(nf)
    ]
    for load in loads:
        load.start()
    own = pltpu.make_async_copy(mix_ref.at[g], got.at[g], own_sem)
    own.start()

    def peer(off):
        to = lax.rem(g + off, group)
        return (sp, to // 2, lax.rem(to, 2))

    greet([(None, peer(off)) for off in range(1, group)])

    def copy(off, to, source):
        return pltpu.make_async_remote_copy(
            mix_ref.at[to],
            got.at[source],
            send.at[off - 1],
            recv.at[off - 1],
            device_id=peer(off),
            device_id_type=MESH,
        )

    for off in range(1, group):
        copy(off, lax.rem(g + off, group), g).start()
    for load in loads:
        load.wait()
    own.wait()

    def add(source, first):
        part = jnp.dot(
            got[source, 0], wbuf[source, 0], preferred_element_type=jnp.float32
        ) + jnp.dot(got[source, 1], wbuf[source, 1], preferred_element_type=jnp.float32)
        acc[...] = part if first else acc[...] + part

    add(g, True)
    for off in range(1, group):
        source = lax.rem(g + group - off, group)
        copy(off, lax.rem(g + off, group), source).wait_recv()
        add(source, False)
    out_ref[...] = acc[...].astype(jnp.bfloat16)
    for off in range(1, group):
        copy(off, lax.rem(g + off, group), g).wait_send()


def exchange_and_merge(mix, wo):
    nf = lax.axis_size("fs")
    group, _, tokens, channels = mix.shape
    width = wo.shape[3]
    vmem = pl.BlockSpec(memory_space=pltpu.VMEM)
    dma = pltpu.SemaphoreType.DMA
    return pl.pallas_call(
        functools.partial(output_kernel, nf),
        out_shape=jax.ShapeDtypeStruct((tokens, width), jnp.bfloat16),
        in_specs=[vmem, pl.BlockSpec(memory_space=pltpu.MemorySpace.HBM)],
        out_specs=vmem,
        scratch_shapes=[
            pltpu.VMEM(mix.shape, jnp.bfloat16),
            pltpu.VMEM(wo.shape, jnp.bfloat16),
            pltpu.VMEM((tokens, width), jnp.float32),
            dma((nf,)),
            dma((group - 1,)),
            dma((group - 1,)),
            dma,
        ],
        compiler_params=pltpu.CompilerParams(
            collective_id=1, has_side_effects=True, vmem_limit_bytes=40 * 1024 * 1024
        ),
    )(mix, wo)


def shards(
    activations,
    norm_gain,
    w_conv_gate,
    w_conv_mult,
    w_conv_in,
    conv_taps,
    w_query,
    w_key,
    w_value,
    w_input_gate,
    w_forget_gate,
    gate_bias,
    decay_shift,
    head_gain,
    w_out_conv,
    w_out_mem,
):
    group_index = lax.axis_index(("fs", "tp"))
    heads_here = MEMORY_HEADS // (lax.axis_size("fs") * lax.axis_size("tp"))
    channels = w_conv_gate.shape[1]
    if lax.axis_size("sp") <= 8 and lax.axis_size("tp") == 2:
        seq_count, tokens = lax.axis_size("fs"), activations.shape[1]
        all_gates = jnp.concatenate([w_input_gate, w_forget_gate], axis=1)
        flat, gate_flat, full_out = gather_and_project(
            activations[0],
            norm_gain[None, :],
            (w_conv_gate, w_conv_mult, w_conv_in, w_query, w_key, w_value),
            all_gates,
            w_out_conv,
            w_out_mem,
        )
        conv_gate, conv_mult, conv_in, query, keys_proj, value = [
            flat[:, at * channels : (at + 1) * channels].reshape(seq_count, tokens, channels)
            for at in range(6)
        ]
        gate_values = jnp.concatenate(
            [
                lax.dynamic_slice_in_dim(
                    gate_flat, at + group_index * heads_here, heads_here, 1
                )
                for at in (0, MEMORY_HEADS)
            ],
            axis=1,
        ).reshape(seq_count, tokens, 2 * heads_here)
    else:
        full_out = None
        sequences = lax.all_gather(activations, "fs", axis=0, tiled=True)
        seq_count = sequences.shape[0]
        tokens = sequences.shape[1]
        model_width = sequences.shape[2]
        row_count = seq_count * tokens
        flat_rows = sequences.reshape(row_count, model_width).astype(jnp.float32)
        normed = (
            flat_rows
            * lax.rsqrt(jnp.mean(flat_rows * flat_rows, axis=-1, keepdims=True) + EPSILON)
            * norm_gain
        ).astype(jnp.bfloat16)
        pieces = (
            lax.all_gather(w_conv_gate, "sp", axis=0, tiled=True),
            lax.all_gather(w_conv_mult, "sp", axis=0, tiled=True),
            lax.all_gather(w_conv_in, "sp", axis=0, tiled=True),
            lax.all_gather(w_query, "sp", axis=0, tiled=True),
            lax.all_gather(w_key, "sp", axis=0, tiled=True),
            lax.all_gather(w_value, "sp", axis=0, tiled=True),
        )
        projected = tuple(
            (jnp.dot(normed, shard_piece, preferred_element_type=jnp.float32) for shard_piece in pieces)
        )
        conv_gate, conv_mult, conv_in, query, keys_proj, value = [
            tensor.astype(jnp.bfloat16).reshape(seq_count, tokens, -1) for tensor in projected
        ]
        entry_cols = lax.dynamic_slice_in_dim(w_input_gate, group_index * heads_here, heads_here, 1)
        forget_cols = lax.dynamic_slice_in_dim(w_forget_gate, group_index * heads_here, heads_here, 1)
        gate_values = jnp.dot(
            normed,
            jnp.concatenate([entry_cols, forget_cols], axis=1),
            preferred_element_type=jnp.float32,
        ).reshape(seq_count, tokens, 2 * heads_here)
    product = (conv_mult.astype(jnp.float32) * conv_in.astype(jnp.float32)).astype(jnp.bfloat16)
    ntaps = conv_taps.shape[0]
    rim_rows = from_behind(product[:, tokens - (ntaps - 1) :, :], "sp", 1)
    padded = jnp.concatenate([rim_rows, product], axis=1).astype(jnp.float32)
    tap_weights = lax.dynamic_slice_in_dim(conv_taps, group_index * channels, channels, 1)
    mixed_sum = jnp.zeros((seq_count, tokens, channels), jnp.float32)
    for tap_index in range(ntaps):
        mixed_sum = (
            mixed_sum + tap_weights[tap_index] * padded[:, tap_index : tap_index + tokens, :]
        )
    conv_out = (conv_gate.astype(jnp.float32) * mixed_sum).astype(jnp.bfloat16)
    bias_rows = lax.dynamic_slice_in_dim(gate_bias, group_index * heads_here, heads_here, 1)
    decay_rows = lax.dynamic_slice_in_dim(decay_shift, group_index * heads_here, heads_here, 2)
    entry = gate_values[..., :heads_here] + bias_rows[0]
    log_forget = jax.nn.log_sigmoid(gate_values[..., heads_here:] + bias_rows[1]) + decay_rows
    cell = memory_cell(
        head_rows(query, seq_count, heads_here),
        head_rows(keys_proj, seq_count, heads_here),
        head_rows(value, seq_count, heads_here),
        gate_rows(entry, seq_count, heads_here),
        gate_rows(log_forget, seq_count, heads_here),
    )
    cell = cell * lax.rsqrt(jnp.mean(cell * cell, axis=-1, keepdims=True) + EPSILON)
    gain_rows = lax.dynamic_slice_in_dim(
        head_gain, group_index * heads_here * HEAD_DIM, heads_here * HEAD_DIM, 0
    ).reshape(1, heads_here, 1, HEAD_DIM)
    scaled = cell.reshape(seq_count, heads_here, tokens, HEAD_DIM) * gain_rows
    mem_out = (
        scaled.transpose(0, 2, 1, 3)
        .reshape(seq_count, tokens, heads_here * HEAD_DIM)
        .astype(jnp.bfloat16)
    )
    if full_out is not None:
        mix = jnp.stack([conv_out, mem_out]).reshape(2, seq_count * 2, tokens // 2, channels)
        merged = exchange_and_merge(mix.transpose(1, 0, 2, 3), full_out)
        return merged[None]
    conv_seq, mem_seq = (
        lax.all_to_all(conv_out, "fs", split_axis=0, concat_axis=2, tiled=True),
        lax.all_to_all(mem_out, "fs", split_axis=0, concat_axis=2, tiled=True),
    )
    rows_conv, rows_mem = (
        lax.all_gather(w_out_conv, "fs", axis=0, tiled=True),
        lax.all_gather(w_out_mem, "fs", axis=0, tiled=True),
    )
    full_conv, full_mem = (
        lax.all_gather(rows_conv, "sp", axis=1, tiled=True),
        lax.all_gather(rows_mem, "sp", axis=1, tiled=True),
    )
    conv_flat = conv_seq[0]
    mem_flat = mem_seq[0]
    output = lax.psum_scatter(
        (
            jnp.dot(conv_flat, full_conv, preferred_element_type=jnp.float32)
            + jnp.dot(mem_flat, full_mem, preferred_element_type=jnp.float32)
        ).astype(jnp.bfloat16),
        "tp",
        scatter_dimension=0,
        tiled=True,
    ).astype(jnp.float32)
    return output.astype(jnp.bfloat16).reshape(1, output.shape[0], -1)


def solution(mesh):
    return jax.shard_map(
        shards,
        mesh=mesh,
        in_specs=(
            P("fs", "sp", None),
            P(),
            P("sp", ("fs", "tp")),
            P("sp", ("fs", "tp")),
            P("sp", ("fs", "tp")),
            P(),
            P("sp", ("fs", "tp")),
            P("sp", ("fs", "tp")),
            P("sp", ("fs", "tp")),
            P(),
            P(),
            P(),
            P(None, "sp", None),
            P(),
            P(("fs", "tp"), "sp"),
            P(("fs", "tp"), "sp"),
        ),
        out_specs=P("fs", ("sp", "tp"), None),
        check_vma=False,
    )
```

```python
import functools

import jax
import jax.numpy as jnp
from jax import lax
from jax.experimental import pallas as pl
from jax.experimental.pallas import tpu as pltpu
from jax.sharding import PartitionSpec as P

MEMORY_HEADS = 8
HEAD_DIM = 128
BLOCK = 64


EPSILON = 1e-06
FAR_BELOW = -1e30
HIGHEST_PRECISION = lax.Precision.HIGHEST


def later_kernel(ns, state_ref, stat_ref, states, stats, s_send, s_recv, t_send, t_recv):
    sp, fs, tp = (lax.axis_index("sp"), lax.axis_index("fs"), lax.axis_index("tp"))
    greet([(None, (lax.rem(sp + off, ns), fs, tp)) for off in range(1, ns)])

    def copies(off, source):
        to = (sp + off, fs, tp)
        return (
            pltpu.make_async_remote_copy(
                stat_ref, stats.at[source], t_send.at[off - 1], t_recv.at[off - 1],
                device_id=to, device_id_type=MESH,
            ),
            pltpu.make_async_remote_copy(
                state_ref, states.at[source], s_send.at[off - 1], s_recv.at[off - 1],
                device_id=to, device_id_type=MESH,
            ),
        )

    for off in range(1, ns):

        @pl.when(sp + off < ns)
        def _():
            for copy in copies(off, sp):
                copy.start()

    for off in range(1, ns):

        @pl.when(sp - off >= 0)
        def _():
            for copy in copies(off, sp - off):
                copy.wait_recv()

    for off in range(1, ns):

        @pl.when(sp + off < ns)
        def _():
            for copy in copies(off, sp):
                copy.wait_send()


def send_later(state, stats, ns):
    vmem = pl.BlockSpec(memory_space=pltpu.VMEM)
    return pl.pallas_call(
        functools.partial(later_kernel, ns),
        out_shape=(
            jax.ShapeDtypeStruct((ns,) + state.shape, state.dtype),
            jax.ShapeDtypeStruct((ns,) + stats.shape, stats.dtype),
        ),
        in_specs=[vmem, vmem],
        out_specs=(vmem, vmem),
        scratch_shapes=[pltpu.SemaphoreType.DMA((ns - 1,))] * 4,
        compiler_params=pltpu.CompilerParams(collective_id=2, has_side_effects=True),
    )(state, stats)


def prefix(value, axis, join, neutral):
    count, mine = (lax.axis_size(axis), lax.axis_index(axis))
    total, peak, state = value
    stats = jnp.stack([total, peak], axis=1)[..., None]
    stats = jnp.broadcast_to(stats, stats.shape[:2] + state.shape[-1:])
    stats = jnp.pad(stats, ((0, 0), (0, 6), (0, 0)))
    if count <= 8:
        states, stats = send_later(state.astype(jnp.bfloat16), stats, count)
        pieces = (stats[:, :, 0, 0], stats[:, :, 1, 0], states.astype(jnp.float32))
    else:
        packed = lax.all_gather(jnp.concatenate([state, stats], axis=1), axis)
        height = state.shape[1]
        pieces = (packed[:, :, height, 0], packed[:, :, height + 1, 0], packed[:, :, :height])
    subtotal = jax.tree.map(
        lambda part, zero: jnp.full_like(part, 0) + jnp.asarray(zero, part.dtype), value, neutral
    )

    def lap(position, subtotal):
        longer = join(subtotal, jax.tree.map(lambda part: part[position], pieces))
        return jax.tree.map(lambda new, old: jnp.where(position < mine, new, old), longer, subtotal)

    if count <= 8:
        for position in range(count - 1):
            subtotal = lap(position, subtotal)
        return subtotal
    return lax.fori_loop(0, count - 1, lap, subtotal)


def from_behind(array, axis, by):
    peers = lax.axis_size(axis)
    pairs = [(i, i + by) for i in range(peers) if 0 <= i + by < peers]
    return lax.ppermute(array, axis, pairs)


def combine_states(earlier, later):
    total_one, peak_one, state_one = earlier
    total_two, peak_two, state_two = later
    peak_new = jnp.maximum(total_two + peak_one, peak_two)
    scale_old = jnp.exp(total_two + peak_one - peak_new)
    scale_new = jnp.exp(peak_two - peak_new)
    return (
        total_one + total_two,
        peak_new,
        scale_old[..., None, None] * state_one + scale_new[..., None, None] * state_two,
    )


def head_rows(values, seq_count, heads_here):
    tokens = values.shape[1]
    split_heads = values.reshape(seq_count, tokens, heads_here, HEAD_DIM).transpose(0, 2, 1, 3)
    return split_heads.reshape(seq_count * heads_here, tokens, HEAD_DIM).astype(jnp.float32)


def gate_rows(values, seq_count, heads_here):
    tokens = values.shape[1]
    return values.transpose(0, 2, 1).reshape(seq_count * heads_here, tokens)


def memory_cell(query_rows, key_rows, value_rows, entry_gate, log_forget):
    members = query_rows.shape[0]
    tokens = query_rows.shape[1]
    head_width = query_rows.shape[2]
    nblocks = tokens // BLOCK
    block_shape = (members, nblocks, BLOCK, head_width)
    query_blocks = query_rows.reshape(block_shape)
    key_blocks = key_rows.reshape(block_shape) * head_width ** (-0.5)
    value_blocks = value_rows.reshape(block_shape)
    entry_blocks = entry_gate.reshape(members, nblocks, BLOCK)
    forget_sums = jnp.cumsum(log_forget.reshape(members, nblocks, BLOCK), axis=-1)
    block_total = forget_sums[..., -1]
    local_logs = block_total[..., None] - forget_sums + entry_blocks
    local_peak = jnp.max(local_logs, axis=-1)
    local_weights = jnp.exp(local_logs - local_peak[..., None])
    local_state = jnp.einsum(
        "bclv,bclk->bcvk",
        local_weights[..., None] * value_blocks,
        key_blocks,
        precision=HIGHEST_PRECISION,
    )

    def advance(running, block_item):
        return (combine_states(running, block_item), running)

    zero_sums = jnp.zeros((members,), jnp.float32)
    low_peaks = jnp.full((members,), FAR_BELOW, jnp.float32)
    zero_states = jnp.zeros((members, head_width, head_width), jnp.float32)
    block_items = (
        jnp.moveaxis(block_total, 1, 0),
        jnp.moveaxis(local_peak, 1, 0),
        jnp.moveaxis(local_state, 1, 0),
    )
    device_total, inner_states = lax.scan(advance, (zero_sums, low_peaks, zero_states), block_items)
    inner_states = tuple((jnp.moveaxis(tensor, 0, 1) for tensor in inner_states))
    total_sum, total_peak, total_state = device_total
    before = prefix(
        (total_sum, total_peak, total_state),
        "sp",
        combine_states,
        (zero_sums, low_peaks, zero_states),
    )
    opening = combine_states((zero_sums, zero_sums, zero_states), before)
    opening = tuple((tensor[:, None] for tensor in opening))
    _, prior_peak, prior_state = combine_states(opening, inner_states)
    positions = jnp.arange(BLOCK)
    causal_mask = positions[:, None] >= positions[None, :]
    pair_logs = jnp.where(
        causal_mask,
        forget_sums[..., :, None] - forget_sums[..., None, :] + entry_blocks[..., None, :],
        -jnp.inf,
    )
    carried_logs = forget_sums + prior_peak[..., None]
    row_peak = jnp.maximum(carried_logs, jnp.max(pair_logs, axis=-1))
    inner_weights = jnp.exp(pair_logs - row_peak[..., None])
    carried_weights = jnp.exp(carried_logs - row_peak)
    scores = inner_weights * jnp.einsum(
        "bcld,bcsd->bcls", query_blocks, key_blocks, precision=HIGHEST_PRECISION
    )
    numerator = carried_weights[..., None] * jnp.einsum(
        "bcvk,bclk->bclv", prior_state, query_blocks, precision=HIGHEST_PRECISION
    ) + jnp.einsum("bcls,bcsv->bclv", scores, value_blocks, precision=HIGHEST_PRECISION)
    return numerator.reshape(members, tokens, head_width)


MESH = pl.DeviceIdType.MESH


def greet(peers):
    barrier = pltpu.get_barrier_semaphore()
    total = 0
    for there, peer in peers:
        if there is None:
            pl.semaphore_signal(barrier, inc=1, device_id=peer, device_id_type=MESH)
            total = total + 1
        else:

            @pl.when(there)
            def _(peer=peer):
                pl.semaphore_signal(barrier, inc=1, device_id=peer, device_id_type=MESH)

            total = total + there.astype(jnp.int32)
    pl.semaphore_wait(barrier, total)


def gather_kernel(
    ns,
    nf,
    cuts,
    act_ref,
    gain_ref,
    w0_ref,
    w1_ref,
    w2_ref,
    w3_ref,
    w4_ref,
    w5_ref,
    wg_ref,
    wc_ref,
    wm_ref,
    proj_ref,
    gate_ref,
    wo_ref,
    acts,
    normed,
    wbuf,
    total,
    local_sem,
    a_send,
    a_recv,
    ad_send,
    ad_recv,
    w_send,
    w_recv,
    o_send,
    o_recv,
    p_send,
    p_recv,
    d_send,
    d_recv,
):
    sp, fs, tp = (lax.axis_index("sp"), lax.axis_index("fs"), lax.axis_index("tp"))
    g = fs * 2 + tp
    depth, cols = w0_ref.shape
    width = 6 * cols
    cut = width // cuts
    tokens, model = act_ref.shape
    half = tokens // 2
    ocols = wc_ref.shape[1]
    partner = (sp, fs, 1 - tp)
    has_up, has_down = (sp + 1 < ns, sp > 0)
    up, down = ((sp + 1, fs, tp), (sp - 1, fs, tp))

    own_rows = pl.ds(pl.multiple_of(sp * depth, depth), depth)
    locals_ = []
    for j, ref in enumerate((w0_ref, w1_ref, w2_ref, w3_ref, w4_ref, w5_ref)):
        locals_.append(
            pltpu.make_async_copy(
                ref, wbuf.at[own_rows, pl.ds(j * cols, cols)], local_sem.at[j]
            )
        )
    own_ocols = pl.ds(pl.multiple_of(sp * ocols, ocols), ocols)
    for m, ref in enumerate((wc_ref, wm_ref)):
        locals_.append(
            pltpu.make_async_copy(ref, wo_ref.at[g, m, :, own_ocols], local_sem.at[6 + m])
        )
    locals_.append(pltpu.make_async_copy(act_ref, acts.at[fs], local_sem.at[8]))
    for copy in locals_:
        copy.start()

    fs_peers = [(None, (sp, lax.rem(fs + off, nf), tp)) for off in range(1, nf)]
    greet(fs_peers + [(None, partner), (has_up, up), (has_down, down)])

    my_half = pl.ds(pl.multiple_of(tp * half, half), half)
    other_half = pl.ds(pl.multiple_of((1 - tp) * half, half), half)

    def act_copy(off, src_f):
        return pltpu.make_async_remote_copy(
            act_ref.at[my_half],
            acts.at[src_f, my_half],
            a_send.at[off - 1],
            a_recv.at[off - 1],
            device_id=(sp, lax.rem(fs + off, nf), tp),
            device_id_type=MESH,
        )

    def act_relay(off, src_f, rows):
        return pltpu.make_async_remote_copy(
            acts.at[src_f, rows],
            acts.at[src_f, rows],
            ad_send.at[off - 1],
            ad_recv.at[off - 1],
            device_id=partner,
            device_id_type=MESH,
        )

    def w_copy(side, d, owner, k):
        rows = pl.ds(pl.multiple_of(owner * depth, depth), depth)
        place = wbuf.at[rows, pl.ds(k * cut, cut)]
        return pltpu.make_async_remote_copy(
            place,
            place,
            w_send.at[side, d, k],
            w_recv.at[side, d, k],
            device_id=(up, down)[side],
            device_id_type=MESH,
        )

    def o_copy(side, d, owner):
        place = wo_ref.at[g, :, :, pl.ds(pl.multiple_of(owner * ocols, ocols), ocols)]
        return pltpu.make_async_remote_copy(
            place,
            place,
            o_send.at[side, d],
            o_recv.at[side, d],
            device_id=(up, down)[side],
            device_id_type=MESH,
        )

    def p_copy(owner, off, src_g):
        place = wo_ref.at[src_g, :, :, pl.ds(pl.multiple_of(owner * ocols, ocols), ocols)]
        return pltpu.make_async_remote_copy(
            place,
            place,
            p_send.at[owner, off - 1],
            p_recv.at[owner, off - 1],
            device_id=(sp, lax.rem(fs + off, nf), tp),
            device_id_type=MESH,
        )

    def d_copy(owner, off, src_g):
        place = wo_ref.at[src_g, :, :, pl.ds(pl.multiple_of(owner * ocols, ocols), ocols)]
        return pltpu.make_async_remote_copy(
            place,
            place,
            d_send.at[owner, off],
            d_recv.at[owner, off],
            device_id=partner,
            device_id_type=MESH,
        )

    def origin(off):
        return lax.rem(fs + nf - off, nf)

    def sends(side, d):
        if side == 0:
            return (sp - d >= 0) & has_up
        return (sp + d < ns) & has_down

    def owner_of(side, d):
        return sp - d if side == 0 else sp + d

    def arrives(side, d):
        return (sp - d >= 0) if side == 0 else (sp + d < ns)

    for off in range(1, nf):
        act_copy(off, fs).start()
    for copy in locals_:
        copy.wait()

    def send_z(side, d):
        @pl.when(sends(side, d))
        def _():
            o_copy(side, d, owner_of(side, d)).start()

    def send_w(side, d, k):
        @pl.when(sends(side, d))
        def _():
            w_copy(side, d, owner_of(side, d), k).start()

    for side in range(2):
        send_z(side, 0)
    for k in range(cuts):
        for side in range(2):
            send_w(side, 0, k)

    def spread(owner):
        for off in range(1, nf):
            p_copy(owner, off, g).start()
        d_copy(owner, 0, g).start()

    spread(sp)
    for off in range(1, nf):
        act_copy(off, origin(off)).wait_recv()
        act_relay(off, origin(off), my_half).start()

    def z_round(d):
        for side in range(2):

            @pl.when(arrives(side, d))
            def _():
                owner = owner_of(side, d)
                o_copy(side, d - 1, owner).wait_recv()
                if d < ns - 1:
                    send_z(side, d)
                spread(owner)

    for off in range(1, nf):
        act_relay(off, origin(off), other_half).wait_recv()

    step = 64

    def norm_rows(i, carry):
        f = i // (tokens // step)
        rows = pl.ds(pl.multiple_of(lax.rem(i, tokens // step) * step, step), step)
        x = acts[f, rows, :].astype(jnp.float32)
        scale = lax.rsqrt(jnp.mean(x * x, axis=-1, keepdims=True) + EPSILON)
        out = (x * scale * gain_ref[...]).astype(jnp.bfloat16)
        normed[pl.ds(pl.multiple_of(i * step, step), step), :] = out
        return carry

    lax.fori_loop(0, nf * tokens // step, norm_rows, 0)
    tile = tokens

    def multiply(owner, first):
        rows = pl.ds(pl.multiple_of(owner * depth, depth), depth)

        def body(i, carry):
            here = pl.ds(pl.multiple_of(i * tile, tile), tile)
            part = jnp.dot(
                normed[here, rows], wbuf[rows, :], preferred_element_type=jnp.float32
            )
            total[here, :] = part if first else total[here, :] + part
            return carry

        lax.fori_loop(0, nf, body, 0)

    z_round(1)
    multiply(sp, True)

    def gates(i, carry):
        here = pl.ds(pl.multiple_of(i * tile, tile), tile)
        gate_ref[here, :] = jnp.dot(
            normed[here, :], wg_ref[...], preferred_element_type=jnp.float32
        )
        return carry

    lax.fori_loop(0, nf, gates, 0)

    def collect(s, carry):
        for off in range(1, nf):
            src_g = origin(off) * 2 + tp
            p_copy(s, off, src_g).wait_recv()
            d_copy(s, off, src_g).start()
        return carry

    for d in range(1, ns):
        if d == ns - 1:
            lax.fori_loop(0, ns, collect, 0)
        for k in range(cuts):
            for side in range(2):

                @pl.when(arrives(side, d))
                def _():
                    w_copy(side, d - 1, owner_of(side, d), k).wait_recv()
                    if d < ns - 1:
                        send_w(side, d, k)

        for side in range(2):

            @pl.when(arrives(side, d))
            def _():
                multiply(owner_of(side, d), False)

        if d + 1 < ns:
            z_round(d + 1)

    def round_rows(i, carry):
        here = pl.ds(pl.multiple_of(i * tile, tile), tile)
        proj_ref[here, :] = total[here, :].astype(jnp.bfloat16)
        return carry

    lax.fori_loop(0, nf, round_rows, 0)

    def finish(s, carry):
        for off in range(nf):
            d_copy(s, off, origin(off) * 2 + 1 - tp).wait_recv()
            d_copy(s, off, origin(off) * 2 + tp).wait_send()
        for off in range(1, nf):
            p_copy(s, off, g).wait_send()
        return carry

    lax.fori_loop(0, ns, finish, 0)
    for off in range(1, nf):
        act_copy(off, fs).wait_send()
        act_relay(off, origin(off), my_half).wait_send()
    for side in range(2):
        for d in range(ns - 1):

            @pl.when(sends(side, d))
            def _():
                o_copy(side, d, owner_of(side, d)).wait_send()
                for k in range(cuts):
                    w_copy(side, d, owner_of(side, d), k).wait_send()


def gather_and_project(act, gain, weights, gate_weights, w_out_conv, w_out_mem):
    ns, nf = (lax.axis_size("sp"), lax.axis_size("fs"))
    tokens, model = act.shape
    depth, cols = weights[0].shape
    rows, ocols = w_out_conv.shape
    count = nf * tokens
    cuts = 2
    vmem = pl.BlockSpec(memory_space=pltpu.VMEM)
    hbm = pl.BlockSpec(memory_space=pltpu.MemorySpace.HBM)
    dma = pltpu.SemaphoreType.DMA
    return pl.pallas_call(
        functools.partial(gather_kernel, ns, nf, cuts),
        out_shape=(
            jax.ShapeDtypeStruct((count, 6 * cols), jnp.bfloat16),
            jax.ShapeDtypeStruct((count, gate_weights.shape[1]), jnp.float32),
            jax.ShapeDtypeStruct((nf * 2, 2, rows, ns * ocols), jnp.bfloat16),
        ),
        in_specs=[hbm, vmem] + [hbm] * 6 + [vmem, hbm, hbm],
        out_specs=(vmem, vmem, pl.BlockSpec(memory_space=pl.ANY)),
        scratch_shapes=[
            pltpu.VMEM((nf, tokens, model), jnp.bfloat16),
            pltpu.VMEM((count, model), jnp.bfloat16),
            pltpu.VMEM((ns * depth, 6 * cols), jnp.bfloat16),
            pltpu.VMEM((count, 6 * cols), jnp.float32),
            dma((9,)),
            dma((nf - 1,)),
            dma((nf - 1,)),
            dma((nf - 1,)),
            dma((nf - 1,)),
            dma((2, ns - 1, cuts)),
            dma((2, ns - 1, cuts)),
            dma((2, ns - 1)),
            dma((2, ns - 1)),
            dma((ns, nf - 1)),
            dma((ns, nf - 1)),
            dma((ns, nf)),
            dma((ns, nf)),
        ],
        compiler_params=pltpu.CompilerParams(
            collective_id=0, has_side_effects=True, vmem_limit_bytes=50 * 1024 * 1024
        ),
    )(act, gain, *weights, gate_weights, w_out_conv, w_out_mem)


def output_kernel(nf, mix_ref, wo_ref, out_ref, got, wbuf, acc, w_sem, send, recv, own_sem):
    sp, fs, tp = (lax.axis_index("sp"), lax.axis_index("fs"), lax.axis_index("tp"))
    group = nf * 2
    g = fs * 2 + tp
    loads = [
        pltpu.make_async_copy(wo_ref.at[pl.ds(i * 2, 2)], wbuf.at[pl.ds(i * 2, 2)], w_sem.at[i])
        for i in range(nf)
    ]
    for load in loads:
        load.start()
    own = pltpu.make_async_copy(mix_ref.at[g], got.at[g], own_sem)
    own.start()

    def peer(off):
        to = lax.rem(g + off, group)
        return (sp, to // 2, lax.rem(to, 2))

    greet([(None, peer(off)) for off in range(1, group)])

    def copy(off, to, source):
        return pltpu.make_async_remote_copy(
            mix_ref.at[to],
            got.at[source],
            send.at[off - 1],
            recv.at[off - 1],
            device_id=peer(off),
            device_id_type=MESH,
        )

    for off in range(1, group):
        copy(off, lax.rem(g + off, group), g).start()
    for load in loads:
        load.wait()
    own.wait()

    def add(source, first):
        part = jnp.dot(
            got[source, 0], wbuf[source, 0], preferred_element_type=jnp.float32
        ) + jnp.dot(got[source, 1], wbuf[source, 1], preferred_element_type=jnp.float32)
        acc[...] = part if first else acc[...] + part

    add(g, True)
    for off in range(1, group):
        source = lax.rem(g + group - off, group)
        copy(off, lax.rem(g + off, group), source).wait_recv()
        add(source, False)
    out_ref[...] = acc[...].astype(jnp.bfloat16)
    for off in range(1, group):
        copy(off, lax.rem(g + off, group), g).wait_send()


def exchange_and_merge(mix, wo):
    nf = lax.axis_size("fs")
    group, _, tokens, channels = mix.shape
    width = wo.shape[3]
    vmem = pl.BlockSpec(memory_space=pltpu.VMEM)
    dma = pltpu.SemaphoreType.DMA
    return pl.pallas_call(
        functools.partial(output_kernel, nf),
        out_shape=jax.ShapeDtypeStruct((tokens, width), jnp.bfloat16),
        in_specs=[vmem, pl.BlockSpec(memory_space=pltpu.MemorySpace.HBM)],
        out_specs=vmem,
        scratch_shapes=[
            pltpu.VMEM(mix.shape, jnp.bfloat16),
            pltpu.VMEM(wo.shape, jnp.bfloat16),
            pltpu.VMEM((tokens, width), jnp.float32),
            dma((nf,)),
            dma((group - 1,)),
            dma((group - 1,)),
            dma,
        ],
        compiler_params=pltpu.CompilerParams(
            collective_id=1, has_side_effects=True, vmem_limit_bytes=40 * 1024 * 1024
        ),
    )(mix, wo)


def shards(
    activations,
    norm_gain,
    w_conv_gate,
    w_conv_mult,
    w_conv_in,
    conv_taps,
    w_query,
    w_key,
    w_value,
    w_input_gate,
    w_forget_gate,
    gate_bias,
    decay_shift,
    head_gain,
    w_out_conv,
    w_out_mem,
):
    group_index = lax.axis_index(("fs", "tp"))
    heads_here = MEMORY_HEADS // (lax.axis_size("fs") * lax.axis_size("tp"))
    channels = w_conv_gate.shape[1]
    if lax.axis_size("sp") <= 8 and lax.axis_size("tp") == 2:
        seq_count, tokens = lax.axis_size("fs"), activations.shape[1]
        all_gates = jnp.concatenate([w_input_gate, w_forget_gate], axis=1)
        flat, gate_flat, full_out = gather_and_project(
            activations[0],
            norm_gain[None, :],
            (w_conv_gate, w_conv_mult, w_conv_in, w_query, w_key, w_value),
            all_gates,
            w_out_conv,
            w_out_mem,
        )
        conv_gate, conv_mult, conv_in, query, keys_proj, value = [
            flat[:, at * channels : (at + 1) * channels].reshape(seq_count, tokens, channels)
            for at in range(6)
        ]
        gate_values = jnp.concatenate(
            [
                lax.dynamic_slice_in_dim(
                    gate_flat, at + group_index * heads_here, heads_here, 1
                )
                for at in (0, MEMORY_HEADS)
            ],
            axis=1,
        ).reshape(seq_count, tokens, 2 * heads_here)
    else:
        full_out = None
        sequences = lax.all_gather(activations, "fs", axis=0, tiled=True)
        seq_count = sequences.shape[0]
        tokens = sequences.shape[1]
        model_width = sequences.shape[2]
        row_count = seq_count * tokens
        flat_rows = sequences.reshape(row_count, model_width).astype(jnp.float32)
        normed = (
            flat_rows
            * lax.rsqrt(jnp.mean(flat_rows * flat_rows, axis=-1, keepdims=True) + EPSILON)
            * norm_gain
        ).astype(jnp.bfloat16)
        pieces = (
            lax.all_gather(w_conv_gate, "sp", axis=0, tiled=True),
            lax.all_gather(w_conv_mult, "sp", axis=0, tiled=True),
            lax.all_gather(w_conv_in, "sp", axis=0, tiled=True),
            lax.all_gather(w_query, "sp", axis=0, tiled=True),
            lax.all_gather(w_key, "sp", axis=0, tiled=True),
            lax.all_gather(w_value, "sp", axis=0, tiled=True),
        )
        projected = tuple(
            (jnp.dot(normed, shard_piece, preferred_element_type=jnp.float32) for shard_piece in pieces)
        )
        conv_gate, conv_mult, conv_in, query, keys_proj, value = [
            tensor.astype(jnp.bfloat16).reshape(seq_count, tokens, -1) for tensor in projected
        ]
        entry_cols = lax.dynamic_slice_in_dim(w_input_gate, group_index * heads_here, heads_here, 1)
        forget_cols = lax.dynamic_slice_in_dim(w_forget_gate, group_index * heads_here, heads_here, 1)
        gate_values = jnp.dot(
            normed,
            jnp.concatenate([entry_cols, forget_cols], axis=1),
            preferred_element_type=jnp.float32,
        ).reshape(seq_count, tokens, 2 * heads_here)
    product = (conv_mult.astype(jnp.float32) * conv_in.astype(jnp.float32)).astype(jnp.bfloat16)
    ntaps = conv_taps.shape[0]
    rim_rows = from_behind(product[:, tokens - (ntaps - 1) :, :], "sp", 1)
    padded = jnp.concatenate([rim_rows, product], axis=1).astype(jnp.float32)
    tap_weights = lax.dynamic_slice_in_dim(conv_taps, group_index * channels, channels, 1)
    mixed_sum = jnp.zeros((seq_count, tokens, channels), jnp.float32)
    for tap_index in range(ntaps):
        mixed_sum = (
            mixed_sum + tap_weights[tap_index] * padded[:, tap_index : tap_index + tokens, :]
        )
    conv_out = (conv_gate.astype(jnp.float32) * mixed_sum).astype(jnp.bfloat16)
    bias_rows = lax.dynamic_slice_in_dim(gate_bias, group_index * heads_here, heads_here, 1)
    decay_rows = lax.dynamic_slice_in_dim(decay_shift, group_index * heads_here, heads_here, 2)
    entry = gate_values[..., :heads_here] + bias_rows[0]
    log_forget = jax.nn.log_sigmoid(gate_values[..., heads_here:] + bias_rows[1]) + decay_rows
    cell = memory_cell(
        head_rows(query, seq_count, heads_here),
        head_rows(keys_proj, seq_count, heads_here),
        head_rows(value, seq_count, heads_here),
        gate_rows(entry, seq_count, heads_here),
        gate_rows(log_forget, seq_count, heads_here),
    )
    cell = cell * lax.rsqrt(jnp.mean(cell * cell, axis=-1, keepdims=True) + EPSILON)
    gain_rows = lax.dynamic_slice_in_dim(
        head_gain, group_index * heads_here * HEAD_DIM, heads_here * HEAD_DIM, 0
    ).reshape(1, heads_here, 1, HEAD_DIM)
    scaled = cell.reshape(seq_count, heads_here, tokens, HEAD_DIM) * gain_rows
    mem_out = (
        scaled.transpose(0, 2, 1, 3)
        .reshape(seq_count, tokens, heads_here * HEAD_DIM)
        .astype(jnp.bfloat16)
    )
    if full_out is not None:
        mix = jnp.stack([conv_out, mem_out]).reshape(2, seq_count * 2, tokens // 2, channels)
        merged = exchange_and_merge(mix.transpose(1, 0, 2, 3), full_out)
        return merged[None]
    conv_seq, mem_seq = (
        lax.all_to_all(conv_out, "fs", split_axis=0, concat_axis=2, tiled=True),
        lax.all_to_all(mem_out, "fs", split_axis=0, concat_axis=2, tiled=True),
    )
    rows_conv, rows_mem = (
        lax.all_gather(w_out_conv, "fs", axis=0, tiled=True),
        lax.all_gather(w_out_mem, "fs", axis=0, tiled=True),
    )
    full_conv, full_mem = (
        lax.all_gather(rows_conv, "sp", axis=1, tiled=True),
        lax.all_gather(rows_mem, "sp", axis=1, tiled=True),
    )
    conv_flat = conv_seq[0]
    mem_flat = mem_seq[0]
    output = lax.psum_scatter(
        (
            jnp.dot(conv_flat, full_conv, preferred_element_type=jnp.float32)
            + jnp.dot(mem_flat, full_mem, preferred_element_type=jnp.float32)
        ).astype(jnp.bfloat16),
        "tp",
        scatter_dimension=0,
        tiled=True,
    ).astype(jnp.float32)
    return output.astype(jnp.bfloat16).reshape(1, output.shape[0], -1)


def solution(mesh):
    return jax.shard_map(
        shards,
        mesh=mesh,
        in_specs=(
            P("fs", "sp", None),
            P(),
            P("sp", ("fs", "tp")),
            P("sp", ("fs", "tp")),
            P("sp", ("fs", "tp")),
            P(),
            P("sp", ("fs", "tp")),
            P("sp", ("fs", "tp")),
            P("sp", ("fs", "tp")),
            P(),
            P(),
            P(),
            P(None, "sp", None),
            P(),
            P(("fs", "tp"), "sp"),
            P(("fs", "tp"), "sp"),
        ),
        out_specs=P("fs", ("sp", "tp"), None),
        check_vma=False,
    )
```
